128 devices in a mesh: sp: 8 (over x, core), tp: 16 (over z, y).
Axes of the slice: x: 4, y: 4, z: 4, core: 2. Of those that a mesh axis runs over, the one named last changes fastest.
Arguments:
- tokens: bfloat16 [4, 2048, 2048], P(None, ('sp', 'tp')), may hold values from -6 to 6
- norm_gain: float32 [2048], replicated, may hold values from 0.5 to 1.5
- entry_projection: bfloat16 [2048, 2048], P(None, 'tp'), may hold values from -0.125 to 0.125
- valve_projection: bfloat16 [2048, 2048], P(None, 'tp'), may hold values from -0.125 to 0.125
- filter_taps: float32 [4, 2048], P(None, 'tp'), may hold values from -3 to 3
- conv_bias: float32 [2048], P('tp'), may hold values from -0.6 to 0.6
- recur_weight: bfloat16 [16, 128, 128], P('tp'), may hold values from -0.5 to 0.5
- recur_bias: float32 [2048], P('tp'), may hold values from -3 to 3
- entry_weight: bfloat16 [16, 128, 128], P('tp'), may hold values from -0.5 to 0.5
- entry_bias: float32 [2048], P('tp'), may hold values from -0.6 to 0.6
- forget_rate: float32 [2048], P('tp'), may hold values from 3.0517578e-05 to 0.25, as said below
- output_weight: bfloat16 [2048, 2048], P('tp'), may hold values from -0.5 to 0.5
Outputs:
- mixed: bfloat16 [4, 2048, 2048], P(None, ('sp', 'tp'))
The draws below stay inside these ranges and needn't reach their ends.
Inputs may be any that keep to these rules, and one draw needn't show every extreme that they name: forget_rate is positive; its even channels lie between 1 / 32768 and 1 / 8192, its odd channels between 1 / 64 and 1 / 4.
All inputs are finite; a program needn't handle non-finite values.
Results may differ from the reference program's by a relative error of at most 0.02.
Values may be sent and summed in bfloat16 or wider, within the bound.
No kernel may reach another device: no remote copies, remote signals or barrier semaphores. Data moves between devices by JAX's collectives and lax.ppermute only.
A program may use at most 64 MiB of HBM per device.

```python
import jax
import jax.numpy as jnp
from jax import lax

D = 2048
D_LRU = 2048
BLOCKS = 16
WIDTH_BLOCK = 128
CONV_W = 4
SEQS = 4
SEQ_LEN = 2048


def draw_forget_rate(key, part):
    minimum_decay_bound = 1.0 / (16.0 * SEQ_LEN)
    slow_ceiling = 1.0 / (4.0 * SEQ_LEN)
    fast_floor = 1.0 / 64.0
    fast_ceiling = 0.25
    fractions = jax.random.uniform(key, (D_LRU,), jnp.float32)
    channel_index = jnp.arange(D_LRU)
    parity = (channel_index % 2).astype(jnp.float32)
    plain_floor = minimum_decay_bound + parity * (fast_floor - minimum_decay_bound)
    plain_ceiling = slow_ceiling + parity * (fast_ceiling - slow_ceiling)
    floor_log = jnp.log(plain_floor)
    ceiling_log = jnp.log(plain_ceiling)
    values = jnp.exp(floor_log + fractions * (ceiling_log - floor_log))
    values = jnp.clip(values, plain_floor, plain_ceiling)
    return values.astype(jnp.float32)


def levels(key, shape, split, low, largest):
    def one(position, shards_of):
        steps = jax.random.uniform(jax.random.fold_in(jax.random.fold_in(key, 6), position), (shards_of,), jnp.float32, low / len(split), largest / len(split))
        return jnp.repeat(jnp.exp(steps), shape[position] // shards_of).reshape((-1,) + (1,) * (len(shape) - position - 1))

    level = one(*split[0])
    for cut in split[1:]:
        level = level * one(*cut)
    return level


def centred(key, shape, width, reach, cuts=(), held_as=jnp.bfloat16):
    level = levels(key, shape, cuts, -0.22, 0.18) if cuts else 1.0
    drawn = jax.random.normal(key, shape, jnp.float32) * width * level
    return jnp.minimum(jnp.maximum(drawn, -reach), reach).astype(held_as)


def setup_inputs(seed: int = 0) -> dict:
    streams_of = jax.random.split(jax.random.key(seed), 13)
    tokens = centred(streams_of[0], (SEQS, SEQ_LEN, D), 1.0, 6.0, ((1, 128),))
    norm_gain = jnp.clip(1.0 + 0.1 * jax.random.normal(streams_of[1], (D,), jnp.float32), 0.5, 1.5)
    entry_projection = centred(streams_of[2], (D, D_LRU), D ** -0.5, 0.125, ((1, 16),))
    valve_projection = centred(streams_of[3], (D, D_LRU), D ** -0.5, 0.125, ((1, 16),))
    filter_taps = centred(streams_of[4], (CONV_W, D_LRU), 0.5, 3.0, ((1, 16),), jnp.float32)
    conv_bias = centred(streams_of[5], (D_LRU,), 0.1, 0.6, ((0, 16),), jnp.float32)
    recur_weight = centred(streams_of[6], (BLOCKS, WIDTH_BLOCK, WIDTH_BLOCK), WIDTH_BLOCK ** -0.5, 0.5, ((0, 16),))
    recur_bias = centred(streams_of[7], (D_LRU,), 0.5, 3.0, ((0, 16),), jnp.float32)
    entry_weight = centred(streams_of[8], (BLOCKS, WIDTH_BLOCK, WIDTH_BLOCK), WIDTH_BLOCK ** -0.5, 0.5, ((0, 16),))
    entry_bias = centred(streams_of[9], (D_LRU,), 0.1, 0.6, ((0, 16),), jnp.float32)
    forget_rate = draw_forget_rate(jax.random.fold_in(streams_of[12], 71), 0)
    output_weight = centred(streams_of[11], (D_LRU, D), (D_LRU // 16) ** -0.5, 0.5, ((0, 16),))
    return dict(tokens=tokens, norm_gain=norm_gain, entry_projection=entry_projection, valve_projection=valve_projection, filter_taps=filter_taps, conv_bias=conv_bias, recur_weight=recur_weight, recur_bias=recur_bias, entry_weight=entry_weight, entry_bias=entry_bias, forget_rate=forget_rate, output_weight=output_weight)


epsilon = 1e-06
gate_power = 8.0

def combine_pair(earlier, latter):
    return (earlier[0] * latter[0], latter[0] * earlier[1] + latter[1])

def block_product(convolved, weight):
    grouped = convolved.astype(jnp.float32).reshape(SEQ_LEN, BLOCKS, WIDTH_BLOCK)
    product = jnp.einsum('lhi,hij->lhj', grouped, weight.astype(jnp.float32), precision=lax.Precision.HIGHEST)
    return product.reshape(SEQ_LEN, D_LRU)

def reference(tokens, norm_gain, entry_projection, valve_projection, filter_taps, conv_bias, recur_weight, recur_bias, entry_weight, entry_bias, forget_rate, output_weight):

    def per_sequence(sequence):
        widened = sequence.astype(jnp.float32)
        scaled = widened * lax.rsqrt(lax.optimization_barrier(jnp.mean(widened * widened, axis=-1, keepdims=True)) + epsilon)
        rescaled_values = (scaled * norm_gain).astype(jnp.bfloat16)
        conv_input = jnp.dot(rescaled_values, entry_projection, preferred_element_type=jnp.float32).astype(jnp.bfloat16)
        gate_logits = jnp.dot(rescaled_values, valve_projection, preferred_element_type=jnp.float32).astype(jnp.bfloat16)
        padded = jnp.pad(conv_input, ((CONV_W - 1, 0), (0, 0))).astype(jnp.float32)
        summed = conv_bias + padded[0:SEQ_LEN] * filter_taps[0]
        for offset in range(1, CONV_W):
            summed = summed + padded[offset:offset + SEQ_LEN] * filter_taps[offset]
        convolved = summed.astype(jnp.bfloat16)
        recur_gate = jax.nn.sigmoid(block_product(convolved, recur_weight) + recur_bias)
        entry_gate = jax.nn.sigmoid(block_product(convolved, entry_weight) + entry_bias)
        log_decay = -gate_power * recur_gate * forget_rate
        decay = jnp.exp(log_decay)
        pushed = jnp.sqrt(-jnp.expm1(2.0 * log_decay)) * (entry_gate * convolved.astype(jnp.float32))
        hidden_state = lax.associative_scan(combine_pair, (decay, pushed), axis=0)[1]
        valved_lines = (hidden_state * jax.nn.silu(gate_logits.astype(jnp.float32))).astype(jnp.bfloat16)
        return jnp.dot(valved_lines, output_weight, preferred_element_type=jnp.float32).astype(jnp.bfloat16)
    return lax.map(per_sequence, tokens)
```

```python
import jax
import jax.numpy as jnp
from jax import lax
from jax.experimental import pallas as pl
from jax.experimental.pallas import tpu as pltpu
from jax.sharding import Mesh
from jax.sharding import PartitionSpec as P


TP = ("z", "y")
SP_TP = ("x", "c", "z", "y")
EPS = 1e-06
GATE_POWER = 8.0
F32 = jnp.float32
BF16 = jnp.bfloat16
HALF = 1024
SHIFTS = (1, -1, 2)
SOURCES = (0, 3, 1, 2)


def shift(value, axis, by):
    size = lax.axis_size(axis)
    return lax.ppermute(value, axis, [(i, (i + by) % size) for i in range(size)])


def spread(value, axis):
    return [shift(value, axis, by) for by in SHIFTS]


def swap_cores(values):
    return [lax.ppermute(v, "c", [(0, 1), (1, 0)]) for v in values]


def full(shape):
    zeros = (0,) * len(shape)
    return pl.BlockSpec(shape, lambda i, idx: zeros)


def call(kernel, idx, ins, outs, scratch=(), specs=None, name=None):
    in_specs = [full(a.shape) for a in ins] if specs is None else specs
    return pl.pallas_call(
        kernel,
        out_shape=[jax.ShapeDtypeStruct(s, d) for s, d in outs],
        grid_spec=pltpu.PrefetchScalarGridSpec(
            num_scalar_prefetch=1,
            grid=(1,),
            in_specs=in_specs,
            out_specs=[full(s) for s, _ in outs],
            scratch_shapes=list(scratch),
        ),
        name=name,
    )(idx, *ins)


def pack_entry_kernel(idx, entry, taps, bias, rw, rb, ew, eb, rate, out):
    out[0:HALF] = entry[...]
    out[HALF : HALF + 128] = jnp.where(idx[1] == 0, rw[0], ew[0])
    rows = jnp.concatenate([taps[...], bias[...], rb[...], eb[...], rate[...]], axis=0)
    high = rows.astype(BF16).astype(F32)
    rest = rows - high
    middle = rest.astype(BF16).astype(F32)
    low = rest - middle
    out[HALF + 128 :] = jnp.concatenate(
        [high, middle, low, jnp.zeros_like(low)], axis=0
    ).astype(BF16)


def pack_rest_kernel(idx, valve, ow, out_v, out_o):
    out_v[...] = valve[...]
    out_o[...] = ow[...]


def norm_kernel(idx, t0, t1, t2, t3, gain, xn, halo):
    y = idx[3]
    g = gain[...]
    for piece, source in zip((t0, t1, t2, t3), SOURCES):
        slot = pl.multiple_of(((y + source) % 4) * 16, 16)
        for s in range(4):
            v = piece[s].astype(F32)
            scale = lax.rsqrt(jnp.mean(v * v, axis=-1, keepdims=True) + EPS)
            n = (v * scale * g).astype(BF16)
            xn[0, s, pl.ds(slot, 16), :] = n[:, :HALF]
            xn[1, s, pl.ds(slot, 16), :] = n[:, HALF:]
    for k in range(2):
        tails = [xn[k, s, 48:64, :].astype(F32)[12:16] for s in range(4)]
        halo[k] = jnp.concatenate(tails, axis=0).astype(BF16)


def both_halves(own, idx):
    c = idx[1]
    first = own[pl.ds(pl.multiple_of(c * HALF, HALF), HALF), :]
    second = own[pl.ds(pl.multiple_of((1 - c) * HALF, HALF), HALF), :]
    return first, second


def gates_kernel(
    idx, xn, halo, entry, taps, bias, rw, rb, ew, eb, rate,
    a1, a2, a3, b1, b2, b3,
    hloc, acum, ends, total,
    pad,
):
    c, z = idx[1], idx[2]
    lhs_a = jnp.concatenate([xn[c].reshape(256, HALF), halo[c]], axis=0)
    lhs_b = jnp.concatenate([xn[1 - c].reshape(256, HALF), halo[1 - c]], axis=0)
    own_a, own_b = both_halves(entry, idx)
    near, far = (a1, a2, a3), (b1, b2, b3)
    us = []
    for wa, wb in (
        ((own_a, a1[0:HALF]), (own_b, b1[0:HALF])),
        ((a2[0:HALF], a3[0:HALF]), (b2[0:HALF], b3[0:HALF])),
    ):
        u = jnp.dot(lhs_a, jnp.concatenate(wa, axis=1), preferred_element_type=F32)
        u = u + jnp.dot(lhs_b, jnp.concatenate(wb, axis=1), preferred_element_type=F32)
        u = u.astype(BF16).astype(F32)
        us += [u[:, :128], u[:, 128:]]
    for j in range(4):
        u = us[j]
        if j == 0:
            p = jnp.concatenate([taps[...], bias[...], rb[...], eb[...], rate[...]], axis=0)
            rwj, ewj = rw[0], ew[0]
        else:
            q = near[j - 1][HALF + 128 :].astype(F32)
            p = q[0:8] + q[8:16] + q[16:24]
            mine, other = near[j - 1][HALF : HALF + 128], far[j - 1][HALF : HALF + 128]
            rwj = jnp.where(c == 0, mine, other)
            ewj = jnp.where(c == 0, other, mine)
        for s in range(4):
            for half in range(2):
                row = s * 64 + half * 32
                pad[j, pl.ds(24 + half * 4 + s, 32, stride=8), :] = u[row : row + 32]
            for k in range(3):
                pad[j, k * 8 + s : k * 8 + s + 1, :] = u[257 + s * 4 + k : 258 + s * 4 + k]
        for k in range(3):
            pad[j, k * 8 + 4 : k * 8 + 8, :] = pad[j, (32 + k) * 8 : (32 + k) * 8 + 4, :]
        conv = p[4:5] + pad[j, 0:256, :] * p[0:1]
        for k in range(1, 4):
            conv = conv + pad[j, k * 8 : k * 8 + 256, :] * p[k : k + 1]
        conv16 = conv.astype(BF16)
        conv = conv16.astype(F32)
        g = jnp.dot(conv16, jnp.concatenate([rwj, ewj], axis=1), preferred_element_type=F32)
        r = jax.nn.sigmoid(g[:, :128] + p[5:6])
        e = jax.nn.sigmoid(g[:, 128:] + p[6:7])
        log_decay = -GATE_POWER * r * p[7:8]
        decay = jnp.exp(log_decay)
        acum[j] = decay
        hloc[j] = jnp.sqrt(-jnp.tanh(log_decay) * (1.0 + decay * decay)) * (e * conv)
    h = [jnp.zeros((8, 128), F32) for _ in range(4)]
    a = [jnp.ones((8, 128), F32) for _ in range(4)]
    for t in range(32):
        for j in range(4):
            step = acum[j, t * 8 : t * 8 + 8, :]
            h[j] = step * h[j] + hloc[j, t * 8 : t * 8 + 8, :]
            a[j] = step * a[j]
            hloc[j, t * 8 : t * 8 + 8, :] = h[j]
            acum[j, t * 8 : t * 8 + 8, :] = a[j]
    for j in range(4):
        ends[0, j] = a[j]
        ends[1, j] = h[j]
        shard = (z + SOURCES[j]) % 4
        total[0, shard] = a[j][0:4] * a[j][4:8]
        total[1, shard] = a[j][4:8] * h[j][0:4] + h[j][4:8]


def output_kernel(
    idx, xn, hloc, acum, ends, entering, valve, va1, va2, va3, vb1, vb2, vb3,
    ow, oa1, oa2, oa3, ob1, ob2, ob3,
    out0, out1, out2, out3,
    hs, gated, wo,
):
    c, z, y = idx[1], idx[2], idx[3]
    wo[0:128] = ow[...]
    for j, (mine, other) in enumerate(((oa1, ob1), (oa2, ob2), (oa3, ob3)), 1):
        wo[pl.ds(pl.multiple_of(j * 128 + c * 64, 64), 64), :] = mine[...]
        wo[pl.ds(pl.multiple_of(j * 128 + (1 - c) * 64, 64), 64), :] = other[...]
    xa = xn[c].reshape(256, HALF)
    xb = xn[1 - c].reshape(256, HALF)
    own_a, own_b = both_halves(valve, idx)
    logits = []
    for wa, wb in (((own_a, va1[...]), (own_b, vb1[...])), ((va2[...], va3[...]), (vb2[...], vb3[...]))):
        u = jnp.dot(xa, jnp.concatenate(wa, axis=1), preferred_element_type=F32)
        u = u + jnp.dot(xb, jnp.concatenate(wb, axis=1), preferred_element_type=F32)
        u = u.astype(BF16).astype(F32)
        logits += [u[:, :128], u[:, 128:]]
    for j in range(4):
        first = entering[(z + SOURCES[j]) % 4]
        second = ends[1, j, 0:4, :] + ends[0, j, 0:4, :] * first
        state = jnp.concatenate([first, second], axis=0)
        h = hloc[j].reshape(32, 8, 128) + acum[j].reshape(32, 8, 128) * state[None]
        hs[j] = h.reshape(256, 128)
        v = logits[j]
        silu = v * jax.nn.sigmoid(v)
        for s in range(4):
            for half in range(2):
                row = s * 64 + half * 32
                hidden = hs[j, pl.ds(half * 4 + s, 32, stride=8), :]
                gated[s, half * 32 : half * 32 + 32, j * 128 : j * 128 + 128] = (
                    hidden * silu[row : row + 32]
                ).astype(BF16)
    rows = []
    for d in (0, 1, 3, 2):
        slot = pl.multiple_of(((y + d) % 4) * 16, 16)
        rows += [gated[s, pl.ds(slot, 16), :] for s in range(4)]
    mixed = jnp.dot(jnp.concatenate(rows, axis=0), wo[...], preferred_element_type=F32)
    out0[...] = mixed[0:64].reshape(4, 16, 2048)
    for k, out in enumerate((out1, out2, out3), 1):
        out[...] = mixed[k * 64 : k * 64 + 64].reshape(4, 16, 2048).astype(BF16)


def after(earlier, later):
    return jnp.stack([earlier[0] * later[0], later[0] * earlier[1] + later[1]])


def enter(total, done):
    nothing = jnp.stack([jnp.ones_like(total[0]), jnp.zeros_like(total[1])])
    state = nothing
    for axis, mirrored in (("z", False), ("z", True), ("c", False), ("x", False), ("x", True)):
        size = lax.axis_size(axis)
        place = lax.axis_index(axis)
        partner = [(i, size - 1 - i if mirrored else i ^ 1) for i in range(size)]
        upper = place >= 2 if mirrored else place % 2 == 1
        other = lax.ppermute(total, axis, partner)
        state = jnp.where(upper, after(other, state), state)
        total = after(jnp.where(upper, other, total), jnp.where(upper, total, other))
        if axis == "z" and mirrored:
            total, *done = lax.optimization_barrier((total, *done))
    return state[1], done


def per_device(
    tokens,
    norm_gain,
    entry_projection,
    valve_projection,
    filter_taps,
    conv_bias,
    recur_weight,
    recur_bias,
    entry_weight,
    entry_bias,
    forget_rate,
    output_weight,
):
    idx = jnp.stack([lax.axis_index(a) for a in SP_TP]).astype(jnp.int32)
    vector = lambda a: a.reshape(1, -1)
    small = (
        filter_taps,
        vector(conv_bias),
        recur_weight,
        vector(recur_bias),
        entry_weight,
        vector(entry_bias),
        vector(forget_rate),
    )
    core_half = lambda rows, columns: pl.BlockSpec((rows, columns), lambda i, ix: (ix[1], 0))

    pieces = spread(tokens, "y")
    (entry_half,) = call(
        pack_entry_kernel,
        idx,
        (entry_projection, *small),
        [((HALF + 160, 128), BF16)],
        specs=[core_half(HALF, 128)] + [full(a.shape) for a in small],
        name="pack_entry",
    )
    entry_near = spread(entry_half, "z")
    entry_far = swap_cores(entry_near)
    xn, halo = call(
        norm_kernel,
        idx,
        (tokens, *pieces, vector(norm_gain)),
        [((2, 4, 64, HALF), BF16), ((2, 16, HALF), BF16)],
        name="norm",
    )
    stretches = 32
    halo_in = lax.ppermute(halo, ("x", "c", "z"), [(i, i + 1) for i in range(stretches - 1)])
    valve_half, output_half = call(
        pack_rest_kernel,
        idx,
        (valve_projection, output_weight),
        [((HALF, 128), BF16), ((64, 2048), BF16)],
        specs=[core_half(HALF, 128), core_half(64, 2048)],
        name="pack_rest",
    )
    halo, valve_half = lax.optimization_barrier((halo, valve_half))
    valve_near = spread(valve_half, "z")
    valve_far = swap_cores(valve_near)
    hloc, acum, ends, total = call(
        gates_kernel,
        idx,
        (xn, halo_in, entry_projection, *small, *entry_near, *entry_far),
        [((4, 256, 128), F32), ((4, 256, 128), F32), ((2, 4, 8, 128), F32), ((2, 4, 4, 128), F32)],
        scratch=[pltpu.VMEM((4, 280, 128), F32)],
        name="gates",
    )
    entering, (output_half,) = enter(total, (output_half,))
    output_near = spread(output_half, "z")
    output_far = swap_cores(output_near)
    own, *parts = call(
        output_kernel,
        idx,
        (
            xn, hloc, acum, ends, entering,
            valve_projection, *valve_near, *valve_far,
            output_weight, *output_near, *output_far,
        ),
        [((4, 16, 2048), F32)] + [((4, 16, 2048), BF16)] * 3,
        scratch=[
            pltpu.VMEM((4, 256, 128), F32),
            pltpu.VMEM((4, 64, 512), BF16),
            pltpu.VMEM((512, 2048), BF16),
        ],
        name="output",
    )
    mixed = own
    for part, by in zip(parts, SHIFTS):
        mixed = mixed + shift(part, "y", by).astype(F32)
    return mixed.astype(BF16)


def solution(mesh):
    finer = Mesh(mesh.devices.reshape(4, 2, 4, 4), SP_TP)
    placed = (
        P(None, SP_TP, None),
        P(),
        P(None, TP),
        P(None, TP),
        P(None, TP),
        P(TP),
        P(TP, None, None),
        P(TP),
        P(TP, None, None),
        P(TP),
        P(TP),
        P(TP, None),
    )
    return jax.shard_map(
        per_device, mesh=finer, in_specs=placed, out_specs=P(None, SP_TP, None), check_vma=False
    )
```

```python
import functools

import jax
import jax.numpy as jnp
from jax import lax
from jax.experimental import pallas as pl
from jax.experimental.pallas import tpu as pltpu
from jax.sharding import Mesh
from jax.sharding import PartitionSpec as P


TP = ("z", "y")
SP_TP = ("x", "c", "z", "y")
EPS = 1e-06
GATE_POWER = 8.0
F32 = jnp.float32
BF16 = jnp.bfloat16
HALF = 1024
SHIFTS = (1, -1, 2)
SOURCES = (0, 3, 1, 2)


def shift(value, axis, by):
    size = lax.axis_size(axis)
    return lax.ppermute(value, axis, [(i, (i + by) % size) for i in range(size)])


def spread(value, axis):
    return [shift(value, axis, by) for by in SHIFTS]


def swap_cores(values):
    return [shift(v, "c", 1) for v in values]


def call(kernel, idx, ins, outs, scratch=(), far=0, to_hbm=False):
    vmem = pl.BlockSpec(memory_space=pltpu.VMEM)
    anywhere = pl.BlockSpec(memory_space=pltpu.HBM)
    hold = jax.ShapeDtypeStruct if to_hbm else pltpu.VMEM
    return pl.pallas_call(
        kernel,
        out_shape=[hold(s, d) for s, d in outs],
        in_specs=[pl.BlockSpec(memory_space=pltpu.SMEM)]
        + [anywhere if k < far else vmem for k in range(len(ins))],
        out_specs=[vmem] * len(outs),
        scratch_shapes=list(scratch),
        compiler_params=pltpu.CompilerParams(vmem_limit_bytes=16 << 20),
    )(
        idx,
        *[
            pltpu.with_memory_space_constraint(a, pltpu.HBM if k < far else pltpu.VMEM)
            for k, a in enumerate(ins)
        ],
    )


def fetch_kernel(
    idx, entry, valve, ow, tokens, gain, taps, bias, rw, rb, ew, eb, rate,
    out_e, out_q, entry_v, valve_v, ow_v, tokens_v, gain_v, rows_v, rw_v, ew_v,
    taps_v, bias_v, rb_v, eb_v, rate_v, sems,
):
    x, c = idx[0], idx[1]
    eighth = 2 * x + c
    moves = (
        (taps, taps_v), (bias, bias_v), (rb, rb_v), (eb, eb_v), (rate, rate_v), (rw, rw_v),
        (ew, ew_v), (entry, entry_v), (valve, valve_v), (ow, ow_v), (tokens, tokens_v),
        (gain, gain_v),
    )
    copies = [pltpu.make_async_copy(a, b, sems.at[k]) for k, (a, b) in enumerate(moves)]
    for copy in copies:
        copy.start()
    for copy in copies:
        copy.wait()
    out_e[0:HALF] = entry_v[pl.ds(pl.multiple_of(c * HALF, HALF), HALF), :]
    out_e[HALF : HALF + 128] = jnp.where(c == 0, rw_v[0], ew_v[0])
    rows = jnp.concatenate([taps_v[...], bias_v[...], rb_v[...], eb_v[...], rate_v[...]], axis=0)
    rows_v[...] = rows
    high = rows.astype(BF16).astype(F32)
    rest = rows - high
    middle = rest.astype(BF16).astype(F32)
    low = rest - middle
    out_e[HALF + 128 :] = jnp.concatenate(
        [high, middle, low, jnp.zeros_like(low)], axis=0
    ).astype(BF16)
    out_q[0:256] = valve_v[pl.ds(pl.multiple_of(eighth * 256, 256), 256), :]
    rows = ow_v[pl.ds(pl.multiple_of(eighth * 16, 16), 16), :]
    for n in range(16):
        out_q[256 + n * 16 : 272 + n * 16] = rows[:, n * 128 : n * 128 + 128]


def join_kernel(idx, q1, q2, q3, out):
    for k, q in enumerate((q1, q2, q3)):
        out[k * 512 : k * 512 + 512] = q[...]


def norm_kernel(idx, t0, t1, t2, t3, gain, xn, halo):
    y = idx[3]
    g = gain[...]
    for piece, source in zip((t0, t1, t2, t3), SOURCES):
        slot = pl.multiple_of(((y + source) % 4) * 16, 16)
        for s in range(4):
            v = piece[s].astype(F32)
            scale = lax.rsqrt(jnp.mean(v * v, axis=-1, keepdims=True) + EPS)
            n = (v * scale * g).astype(BF16)
            xn[0, s, pl.ds(slot, 16), :] = n[:, :HALF]
            xn[1, s, pl.ds(slot, 16), :] = n[:, HALF:]
    for k in range(2):
        tails = [xn[k, s, 48:64, :].astype(F32)[12:16] for s in range(4)]
        halo[k] = jnp.concatenate(tails, axis=0).astype(BF16)


def both_halves(own, idx):
    c = idx[1]
    first = own[pl.ds(pl.multiple_of(c * HALF, HALF), HALF), :]
    second = own[pl.ds(pl.multiple_of((1 - c) * HALF, HALF), HALF), :]
    return first, second


def gates_kernel(
    idx, xn, halo, entry, own_rows, rw, ew,
    a1, a2, a3, b1, b2, b3,
    hloc, acum, ends, total,
    pad,
):
    c, z = idx[1], idx[2]
    lhs_a = jnp.concatenate([xn[c].reshape(256, HALF), halo[c]], axis=0)
    lhs_b = jnp.concatenate([xn[1 - c].reshape(256, HALF), halo[1 - c]], axis=0)
    own_a, own_b = both_halves(entry, idx)
    near, far = (a1, a2, a3), (b1, b2, b3)
    us = []
    for wa, wb in (
        ((own_a, a1[0:HALF]), (own_b, b1[0:HALF])),
        ((a2[0:HALF], a3[0:HALF]), (b2[0:HALF], b3[0:HALF])),
    ):
        u = jnp.dot(lhs_a, jnp.concatenate(wa, axis=1), preferred_element_type=F32)
        u = u + jnp.dot(lhs_b, jnp.concatenate(wb, axis=1), preferred_element_type=F32)
        u = u.astype(BF16).astype(F32)
        us += [u[:, :128], u[:, 128:]]
    for j in range(4):
        u = us[j]
        if j == 0:
            p = own_rows[...]
            rwj, ewj = rw[0], ew[0]
        else:
            q = near[j - 1][HALF + 128 :].astype(F32)
            p = q[0:8] + q[8:16] + q[16:24]
            mine, other = near[j - 1][HALF : HALF + 128], far[j - 1][HALF : HALF + 128]
            rwj = jnp.where(c == 0, mine, other)
            ewj = jnp.where(c == 0, other, mine)
        for s in range(4):
            for half in range(2):
                row = s * 64 + half * 32
                pad[j, pl.ds(24 + half * 4 + s, 32, stride=8), :] = u[row : row + 32]
            for k in range(3):
                pad[j, k * 8 + s : k * 8 + s + 1, :] = u[257 + s * 4 + k : 258 + s * 4 + k]
        for k in range(3):
            pad[j, k * 8 + 4 : k * 8 + 8, :] = pad[j, (32 + k) * 8 : (32 + k) * 8 + 4, :]
        conv = p[4:5] + pad[j, 0:256, :] * p[0:1]
        for k in range(1, 4):
            conv = conv + pad[j, k * 8 : k * 8 + 256, :] * p[k : k + 1]
        conv16 = conv.astype(BF16)
        conv = conv16.astype(F32)
        g = jnp.dot(conv16, jnp.concatenate([rwj, ewj], axis=1), preferred_element_type=F32)
        r = jax.nn.sigmoid(g[:, :128] + p[5:6])
        e = jax.nn.sigmoid(g[:, 128:] + p[6:7])
        log_decay = -GATE_POWER * r * p[7:8]
        decay = jnp.exp(log_decay)
        acum[j] = decay
        hloc[j] = jnp.sqrt(-jnp.tanh(log_decay) * (1.0 + decay * decay)) * (e * conv)
    h = [jnp.zeros((8, 128), F32) for _ in range(4)]
    a = [jnp.ones((8, 128), F32) for _ in range(4)]
    for t in range(32):
        for j in range(4):
            step = acum[j, t * 8 : t * 8 + 8, :]
            h[j] = step * h[j] + hloc[j, t * 8 : t * 8 + 8, :]
            a[j] = step * a[j]
            hloc[j, t * 8 : t * 8 + 8, :] = h[j]
            acum[j, t * 8 : t * 8 + 8, :] = a[j]
    for j in range(4):
        ends[0, j] = a[j]
        ends[1, j] = h[j]
        shard = (z + SOURCES[j]) % 4
        total[0, shard] = a[j][0:4] * a[j][4:8]
        total[1, shard] = a[j][4:8] * h[j][0:4] + h[j][4:8]


def prepare_kernel(idx, xn, valve, ow, g0, g1, g2, g3, f0, f1, f2, f3, silu, wo, wv):
    x, c = idx[0], idx[1]
    wv[:, 0:128] = valve[...]
    wo[0:128] = ow[...]
    for m, (mine, other) in enumerate(((g0, f0), (g1, f1), (g2, f2), (g3, f3))):
        for core, piece in ((c, mine), (1 - c, other)):
            eighth = ((x + SOURCES[m]) % 4) * 2 + core
            for j in range(1, 4):
                top = (j - 1) * 512
                wv[pl.ds(pl.multiple_of(eighth * 256, 256), 256), j * 128 : j * 128 + 128] = piece[
                    top : top + 256
                ]
                row = pl.multiple_of(j * 128 + eighth * 16, 16)
                for n in range(16):
                    wo[pl.ds(row, 16), n * 128 : n * 128 + 128] = piece[
                        top + 256 + n * 16 : top + 272 + n * 16
                    ]
    u = jnp.dot(xn[0].reshape(256, HALF), wv[0:HALF], preferred_element_type=F32)
    u = u + jnp.dot(xn[1].reshape(256, HALF), wv[HALF:], preferred_element_type=F32)
    u = u.astype(BF16).astype(F32)
    silu[...] = u * jax.nn.sigmoid(u)


def output_kernel(
    idx, hloc, acum, ends, entering, silu, wo, out0, out1, out2, out3, hs, gated
):
    z, y = idx[2], idx[3]
    for j in range(4):
        first = entering[(z + SOURCES[j]) % 4]
        second = ends[1, j, 0:4, :] + ends[0, j, 0:4, :] * first
        state = jnp.concatenate([first, second], axis=0)
        h = hloc[j].reshape(32, 8, 128) + acum[j].reshape(32, 8, 128) * state[None]
        hs[j] = h.reshape(256, 128)
        for s in range(4):
            for half in range(2):
                row = s * 64 + half * 32
                hidden = hs[j, pl.ds(half * 4 + s, 32, stride=8), :]
                gated[s, half * 32 : half * 32 + 32, j * 128 : j * 128 + 128] = (
                    hidden * silu[row : row + 32, j * 128 : j * 128 + 128]
                ).astype(BF16)
    rows = []
    for d in (0, 1, 3, 2):
        slot = pl.multiple_of(((y + d) % 4) * 16, 16)
        rows += [gated[s, pl.ds(slot, 16), :] for s in range(4)]
    mixed = jnp.dot(jnp.concatenate(rows, axis=0), wo[...], preferred_element_type=F32)
    out0[...] = mixed[0:64].reshape(4, 16, 2048)
    for k, out in enumerate((out1, out2, out3), 1):
        out[...] = mixed[k * 64 : k * 64 + 64].reshape(4, 16, 2048).astype(BF16)


def mix_kernel(idx, own, r1, r2, r3, out):
    total = own[...] + r1[...].astype(F32) + r2[...].astype(F32) + r3[...].astype(F32)
    out[...] = total.astype(BF16)


def after(earlier, later):
    return earlier[0] * later[0], later[0] * earlier[1] + later[1]


def level_kernel(idx, total, other, *rest, position, mirrored, first, last):
    state = None if first else rest[0]
    out = rest if first else rest[1:]
    place = idx[position]
    upper = (place >= 2) if mirrored else (place % 2 == 1)
    mine = (total[0], total[1])
    theirs = (other[0], other[1])
    if first:
        new = [jnp.where(upper, theirs[0], 1.0), jnp.where(upper, theirs[1], 0.0)]
    else:
        old = (state[0], state[1])
        new = [jnp.where(upper, n, o) for n, o in zip(after(theirs, old), old)]
    if last:
        out[0][...] = new[1]
        return
    out[0][0], out[0][1] = new
    earlier = [jnp.where(upper, t, m) for t, m in zip(theirs, mine)]
    later = [jnp.where(upper, m, t) for t, m in zip(theirs, mine)]
    out[1][0], out[1][1] = after(earlier, later)


def enter(total, idx):
    levels = (("z", False), ("z", True), ("c", False), ("x", False), ("x", True))
    state = None
    for k, (axis, mirrored) in enumerate(levels):
        size = lax.axis_size(axis)
        partner = [(i, size - 1 - i if mirrored else i ^ 1) for i in range(size)]
        other = lax.ppermute(total, axis, partner)
        first, last = k == 0, k == len(levels) - 1
        kernel = functools.partial(
            level_kernel,
            position=SP_TP.index(axis),
            mirrored=mirrored,
            first=first,
            last=last,
        )
        pair = ((2, 4, 4, 128), F32)
        outs = [((4, 4, 128), F32)] if last else [pair, pair]
        ins = (total, other) if first else (total, other, state)
        state, *left = call(kernel, idx, ins, outs)
        total = left[0] if left else None
    return state


def per_device(
    tokens,
    norm_gain,
    entry_projection,
    valve_projection,
    filter_taps,
    conv_bias,
    recur_weight,
    recur_bias,
    entry_weight,
    entry_bias,
    forget_rate,
    output_weight,
):
    idx = jnp.stack([lax.axis_index(a) for a in SP_TP]).astype(jnp.int32)
    vector = lambda a: a.reshape(1, -1)
    small = (
        filter_taps,
        vector(conv_bias),
        recur_weight,
        vector(recur_bias),
        entry_weight,
        vector(entry_bias),
        vector(forget_rate),
    )
    pieces = spread(tokens, "y")
    gate = ((1, 128, 128), BF16)
    message, eighths, entry, valve, ow, own_tokens, gain, rows, rw, ew = call(
        fetch_kernel,
        idx,
        (entry_projection, valve_projection, output_weight, tokens, vector(norm_gain), *small),
        [
            ((HALF + 160, 128), BF16), ((512, 128), BF16), ((2048, 128), BF16),
            ((2048, 128), BF16), ((128, 2048), BF16), ((4, 16, 2048), BF16), ((1, 2048), F32),
            ((8, 128), F32), gate, gate,
        ],
        scratch=[pltpu.VMEM((4, 128), F32)]
        + [pltpu.VMEM((1, 128), F32)] * 4
        + [pltpu.SemaphoreType.DMA((12,))],
        far=12,
    )
    quarters = spread(eighths, "z")
    entry_near = spread(message, "z")
    (joined,) = call(join_kernel, idx, quarters, [((1536, 128), BF16)])
    gathered = [joined] + spread(joined, "x")
    xn, halo = call(
        norm_kernel,
        idx,
        (own_tokens, *pieces, gain),
        [((2, 4, 64, HALF), BF16), ((2, 16, HALF), BF16)],
    )
    stretches = 32
    halo_in = lax.ppermute(halo, ("x", "c", "z"), [(i, i + 1) for i in range(stretches - 1)])
    entry_far = swap_cores(entry_near)
    gathered_far = swap_cores(gathered)
    hloc, acum, ends, total = call(
        gates_kernel,
        idx,
        (xn, halo_in, entry, rows, rw, ew, *entry_near, *entry_far),
        [((4, 256, 128), F32), ((4, 256, 128), F32), ((2, 4, 8, 128), F32), ((2, 4, 4, 128), F32)],
        scratch=[pltpu.VMEM((4, 280, 128), F32)],
    )
    entering = enter(total, idx)
    silu, wo = call(
        prepare_kernel,
        idx,
        (xn, valve, ow, *gathered, *gathered_far),
        [((256, 512), F32), ((512, 2048), BF16)],
        scratch=[pltpu.VMEM((2048, 512), BF16)],
    )
    own, *parts = call(
        output_kernel,
        idx,
        (hloc, acum, ends, entering, silu, wo),
        [((4, 16, 2048), F32)] + [((4, 16, 2048), BF16)] * 3,
        scratch=[pltpu.VMEM((4, 256, 128), F32), pltpu.VMEM((4, 64, 512), BF16)],
    )
    parts = [shift(p, "y", by) for p, by in zip(parts, SHIFTS)]
    (mixed,) = call(mix_kernel, idx, (own, *parts), [((4, 16, 2048), BF16)], to_hbm=True)
    return mixed


def solution(mesh):
    finer = Mesh(mesh.devices.reshape(4, 2, 4, 4), SP_TP)
    placed = (
        P(None, SP_TP, None),
        P(),
        P(None, TP),
        P(None, TP),
        P(None, TP),
        P(TP),
        P(TP, None, None),
        P(TP),
        P(TP, None, None),
        P(TP),
        P(TP),
        P(TP, None),
    )

    return jax.shard_map(
        per_device, mesh=finer, in_specs=placed, out_specs=P(None, SP_TP, None), check_vma=False
    )
```

```python
import functools

import jax
import jax.numpy as jnp
from jax import lax
from jax.experimental import pallas as pl
from jax.experimental.pallas import tpu as pltpu
from jax.sharding import Mesh
from jax.sharding import PartitionSpec as P


TP = ("z", "y")
SP_TP = ("x", "c", "z", "y")
EPS = 1e-06
GATE_POWER = 8.0
F32 = jnp.float32
BF16 = jnp.bfloat16
HALF = 1024
SHIFTS = (1, -1, 2)
SOURCES = (0, 3, 1, 2)


def shift(value, axis, by):
    size = lax.axis_size(axis)
    return lax.ppermute(value, axis, [(i, (i + by) % size) for i in range(size)])


def spread(value, axis):
    return [shift(value, axis, by) for by in SHIFTS]


def swap_cores(values):
    return [shift(v, "c", 1) for v in values]


def call(kernel, idx, ins, outs, scratch=(), far=0, to_hbm=False):
    vmem = pl.BlockSpec(memory_space=pltpu.VMEM)
    anywhere = pl.BlockSpec(memory_space=pltpu.HBM)
    hold = jax.ShapeDtypeStruct if to_hbm else pltpu.VMEM
    place = () if idx is None else (idx,)
    return pl.pallas_call(
        kernel,
        out_shape=[hold(s, d) for s, d in outs],
        in_specs=[pl.BlockSpec(memory_space=pltpu.SMEM)] * len(place)
        + [anywhere if k < far else vmem for k in range(len(ins))],
        out_specs=[vmem] * len(outs),
        scratch_shapes=list(scratch),
        compiler_params=pltpu.CompilerParams(vmem_limit_bytes=16 << 20),
    )(
        *place,
        *[
            pltpu.with_memory_space_constraint(a, pltpu.HBM if k < far else pltpu.VMEM)
            for k, a in enumerate(ins)
        ],
    )


def fetch_kernel(
    idx, entry, valve, ow, tokens, gain, taps, bias, rw, rb, ew, eb, rate,
    out_e, out_q, entry_v, valve_v, ow_v, tokens_v, gain_v, rows_v, rw_v, ew_v, flags,
    taps_v, bias_v, rb_v, eb_v, rate_v, sems,
):
    x, c = idx[0], idx[1]
    eighth = 2 * x + c
    moves = (
        (taps, taps_v), (bias, bias_v), (rb, rb_v), (eb, eb_v), (rate, rate_v), (rw, rw_v),
        (ew, ew_v), (entry, entry_v), (valve, valve_v), (ow, ow_v), (tokens, tokens_v),
        (gain, gain_v),
    )
    copies = [pltpu.make_async_copy(a, b, sems.at[k]) for k, (a, b) in enumerate(moves)]
    for copy in copies:
        copy.start()
    for copy in copies:
        copy.wait()
    flag = lax.broadcasted_iota(jnp.int32, (8, 128), 0)
    x_at, c_at, z_at = idx[0], idx[1], idx[2]
    signs = (z_at % 2, z_at // 2, c_at, x_at % 2, x_at // 2)
    value = jnp.zeros((8, 128), jnp.int32)
    for k, sign in enumerate(signs):
        value = jnp.where(flag == k, sign, value)
    flags[...] = value.astype(F32)
    out_e[0:HALF] = entry_v[pl.ds(pl.multiple_of(c * HALF, HALF), HALF), :]
    out_e[HALF : HALF + 128] = jnp.where(c == 0, rw_v[0], ew_v[0])
    rows = jnp.concatenate([taps_v[...], bias_v[...], rb_v[...], eb_v[...], rate_v[...]], axis=0)
    rows_v[...] = rows
    high = rows.astype(BF16).astype(F32)
    rest = rows - high
    middle = rest.astype(BF16).astype(F32)
    low = rest - middle
    out_e[HALF + 128 :] = jnp.concatenate(
        [high, middle, low, jnp.zeros_like(low)], axis=0
    ).astype(BF16)
    out_q[0:256] = valve_v[pl.ds(pl.multiple_of(eighth * 256, 256), 256), :]
    rows = ow_v[pl.ds(pl.multiple_of(eighth * 16, 16), 16), :]
    for n in range(16):
        out_q[256 + n * 16 : 272 + n * 16] = rows[:, n * 128 : n * 128 + 128]


def join_kernel(q1, q2, q3, out):
    for k, q in enumerate((q1, q2, q3)):
        out[k * 512 : k * 512 + 512] = q[...]


def norm_kernel(idx, t0, t1, t2, t3, gain, xn, halo):
    y = idx[3]
    g = gain[...]
    for piece, source in zip((t0, t1, t2, t3), SOURCES):
        slot = pl.multiple_of(((y + source) % 4) * 16, 16)
        for s in range(4):
            v = piece[s].astype(F32)
            scale = lax.rsqrt(jnp.mean(v * v, axis=-1, keepdims=True) + EPS)
            n = (v * scale * g).astype(BF16)
            xn[0, s, pl.ds(slot, 16), :] = n[:, :HALF]
            xn[1, s, pl.ds(slot, 16), :] = n[:, HALF:]
    for k in range(2):
        tails = [xn[k, s, 48:64, :].astype(F32)[12:16] for s in range(4)]
        halo[k] = jnp.concatenate(tails, axis=0).astype(BF16)


def both_halves(own, idx):
    c = idx[1]
    first = own[pl.ds(pl.multiple_of(c * HALF, HALF), HALF), :]
    second = own[pl.ds(pl.multiple_of((1 - c) * HALF, HALF), HALF), :]
    return first, second


def gates_kernel(
    idx, xn, halo, entry, own_rows, rw, ew,
    a1, a2, a3, b1, b2, b3,
    hloc, acum, ends, total,
    pad,
):
    c, z = idx[1], idx[2]
    lhs_a = jnp.concatenate([xn[c].reshape(256, HALF), halo[c]], axis=0)
    lhs_b = jnp.concatenate([xn[1 - c].reshape(256, HALF), halo[1 - c]], axis=0)
    own_a, own_b = both_halves(entry, idx)
    near, far = (a1, a2, a3), (b1, b2, b3)
    us = []
    for wa, wb in (
        ((own_a, a1[0:HALF]), (own_b, b1[0:HALF])),
        ((a2[0:HALF], a3[0:HALF]), (b2[0:HALF], b3[0:HALF])),
    ):
        u = jnp.dot(lhs_a, jnp.concatenate(wa, axis=1), preferred_element_type=F32)
        u = u + jnp.dot(lhs_b, jnp.concatenate(wb, axis=1), preferred_element_type=F32)
        u = u.astype(BF16).astype(F32)
        us += [u[:, :128], u[:, 128:]]
    for j in range(4):
        u = us[j]
        if j == 0:
            p = own_rows[...]
            rwj, ewj = rw[0], ew[0]
        else:
            q = near[j - 1][HALF + 128 :].astype(F32)
            p = q[0:8] + q[8:16] + q[16:24]
            mine, other = near[j - 1][HALF : HALF + 128], far[j - 1][HALF : HALF + 128]
            rwj = jnp.where(c == 0, mine, other)
            ewj = jnp.where(c == 0, other, mine)
        for s in range(4):
            for half in range(2):
                row = s * 64 + half * 32
                pad[j, pl.ds(24 + half * 4 + s, 32, stride=8), :] = u[row : row + 32]
            for k in range(3):
                pad[j, k * 8 + s : k * 8 + s + 1, :] = u[257 + s * 4 + k : 258 + s * 4 + k]
        for k in range(3):
            pad[j, k * 8 + 4 : k * 8 + 8, :] = pad[j, (32 + k) * 8 : (32 + k) * 8 + 4, :]
        conv = p[4:5] + pad[j, 0:256, :] * p[0:1]
        for k in range(1, 4):
            conv = conv + pad[j, k * 8 : k * 8 + 256, :] * p[k : k + 1]
        conv16 = conv.astype(BF16)
        conv = conv16.astype(F32)
        g = jnp.dot(conv16, jnp.concatenate([rwj, ewj], axis=1), preferred_element_type=F32)
        r = jax.nn.sigmoid(g[:, :128] + p[5:6])
        e = jax.nn.sigmoid(g[:, 128:] + p[6:7])
        log_decay = -GATE_POWER * r * p[7:8]
        decay = jnp.exp(log_decay)
        acum[j] = decay
        hloc[j] = jnp.sqrt(-jnp.tanh(log_decay) * (1.0 + decay * decay)) * (e * conv)
    h = [jnp.zeros((8, 128), F32) for _ in range(4)]
    a = [jnp.ones((8, 128), F32) for _ in range(4)]
    for t in range(32):
        for j in range(4):
            step = acum[j, t * 8 : t * 8 + 8, :]
            h[j] = step * h[j] + hloc[j, t * 8 : t * 8 + 8, :]
            a[j] = step * a[j]
            hloc[j, t * 8 : t * 8 + 8, :] = h[j]
            acum[j, t * 8 : t * 8 + 8, :] = a[j]
    for j in range(4):
        ends[0, j] = a[j]
        ends[1, j] = h[j]
        shard = (z + SOURCES[j]) % 4
        total[0, shard] = a[j][0:4] * a[j][4:8]
        total[1, shard] = a[j][4:8] * h[j][0:4] + h[j][4:8]


def prepare_kernel(idx, xn, valve, ow, g0, g1, g2, g3, f0, f1, f2, f3, silu, wo, wv):
    x, c = idx[0], idx[1]
    wv[:, 0:128] = valve[...]
    wo[0:128] = ow[...]
    for m, (mine, other) in enumerate(((g0, f0), (g1, f1), (g2, f2), (g3, f3))):
        for core, piece in ((c, mine), (1 - c, other)):
            eighth = ((x + SOURCES[m]) % 4) * 2 + core
            for j in range(1, 4):
                top = (j - 1) * 512
                wv[pl.ds(pl.multiple_of(eighth * 256, 256), 256), j * 128 : j * 128 + 128] = piece[
                    top : top + 256
                ]
                row = pl.multiple_of(j * 128 + eighth * 16, 16)
                for n in range(16):
                    wo[pl.ds(row, 16), n * 128 : n * 128 + 128] = piece[
                        top + 256 + n * 16 : top + 272 + n * 16
                    ]
    u = jnp.dot(xn[0].reshape(256, HALF), wv[0:HALF], preferred_element_type=F32)
    u = u + jnp.dot(xn[1].reshape(256, HALF), wv[HALF:], preferred_element_type=F32)
    u = u.astype(BF16).astype(F32)
    silu[...] = u * jax.nn.sigmoid(u)


def output_kernel(
    idx, hloc, acum, ends, entering, silu, wo, out0, out1, out2, out3, hs, gated
):
    z, y = idx[2], idx[3]
    for j in range(4):
        first = entering[(z + SOURCES[j]) % 4]
        second = ends[1, j, 0:4, :] + ends[0, j, 0:4, :] * first
        state = jnp.concatenate([first, second], axis=0)
        h = hloc[j].reshape(32, 8, 128) + acum[j].reshape(32, 8, 128) * state[None]
        hs[j] = h.reshape(256, 128)
        for s in range(4):
            for half in range(2):
                row = s * 64 + half * 32
                hidden = hs[j, pl.ds(half * 4 + s, 32, stride=8), :]
                gated[s, half * 32 : half * 32 + 32, j * 128 : j * 128 + 128] = (
                    hidden * silu[row : row + 32, j * 128 : j * 128 + 128]
                ).astype(BF16)
    rows = []
    for d in (0, 1, 3, 2):
        slot = pl.multiple_of(((y + d) % 4) * 16, 16)
        rows += [gated[s, pl.ds(slot, 16), :] for s in range(4)]
    mixed = jnp.dot(jnp.concatenate(rows, axis=0), wo[...], preferred_element_type=F32)
    out0[...] = mixed[0:64].reshape(4, 16, 2048)
    for k, out in enumerate((out1, out2, out3), 1):
        out[...] = mixed[k * 64 : k * 64 + 64].reshape(4, 16, 2048).astype(BF16)


def mix_kernel(own, r1, r2, r3, out):
    total = own[...] + r1[...].astype(F32) + r2[...].astype(F32) + r3[...].astype(F32)
    out[...] = total.astype(BF16)


def after(earlier, later):
    return earlier[0] * later[0], later[0] * earlier[1] + later[1]


def level_kernel(flags, total, other, *rest, level, first, last):
    state = None if first else rest[0]
    out = rest if first else rest[1:]
    upper = jnp.broadcast_to(flags[level : level + 1, :].reshape(1, 1, 128), (4, 4, 128)) > 0.5
    mine = (total[0], total[1])
    theirs = (other[0], other[1])
    if first:
        new = [jnp.where(upper, theirs[0], 1.0), jnp.where(upper, theirs[1], 0.0)]
    else:
        old = (state[0], state[1])
        new = [jnp.where(upper, n, o) for n, o in zip(after(theirs, old), old)]
    if last:
        out[0][...] = new[1]
        return
    out[0][0], out[0][1] = new
    earlier = [jnp.where(upper, t, m) for t, m in zip(theirs, mine)]
    later = [jnp.where(upper, m, t) for t, m in zip(theirs, mine)]
    out[1][0], out[1][1] = after(earlier, later)


def enter(total, flags):
    levels = (("z", False), ("z", True), ("c", False), ("x", False), ("x", True))
    state = None
    for k, (axis, mirrored) in enumerate(levels):
        size = lax.axis_size(axis)
        partner = [(i, size - 1 - i if mirrored else i ^ 1) for i in range(size)]
        other = lax.ppermute(total, axis, partner)
        first, last = k == 0, k == len(levels) - 1
        kernel = functools.partial(
            level_kernel,
            level=k,
            first=first,
            last=last,
        )
        pair = ((2, 4, 4, 128), F32)
        outs = [((4, 4, 128), F32)] if last else [pair, pair]
        ins = (flags, total, other) if first else (flags, total, other, state)
        state, *left = call(kernel, None, ins, outs)
        total = left[0] if left else None
    return state


def per_device(
    tokens,
    norm_gain,
    entry_projection,
    valve_projection,
    filter_taps,
    conv_bias,
    recur_weight,
    recur_bias,
    entry_weight,
    entry_bias,
    forget_rate,
    output_weight,
):
    idx = jnp.stack([lax.axis_index(a) for a in SP_TP]).astype(jnp.int32)
    vector = lambda a: a.reshape(1, -1)
    small = (
        filter_taps,
        vector(conv_bias),
        recur_weight,
        vector(recur_bias),
        entry_weight,
        vector(entry_bias),
        vector(forget_rate),
    )
    pieces = spread(tokens, "y")
    gate = ((1, 128, 128), BF16)
    message, eighths, entry, valve, ow, own_tokens, gain, rows, rw, ew, flags = call(
        fetch_kernel,
        idx,
        (entry_projection, valve_projection, output_weight, tokens, vector(norm_gain), *small),
        [
            ((HALF + 160, 128), BF16), ((512, 128), BF16), ((2048, 128), BF16),
            ((2048, 128), BF16), ((128, 2048), BF16), ((4, 16, 2048), BF16), ((1, 2048), F32),
            ((8, 128), F32), gate, gate, ((8, 128), F32),
        ],
        scratch=[pltpu.VMEM((4, 128), F32)]
        + [pltpu.VMEM((1, 128), F32)] * 4
        + [pltpu.SemaphoreType.DMA((12,))],
        far=12,
    )
    quarters = spread(eighths, "z")
    entry_near = spread(message, "z")
    (joined,) = call(join_kernel, None, quarters, [((1536, 128), BF16)])
    gathered = [joined] + spread(joined, "x")
    xn, halo = call(
        norm_kernel,
        idx,
        (own_tokens, *pieces, gain),
        [((2, 4, 64, HALF), BF16), ((2, 16, HALF), BF16)],
    )
    stretches = 32
    halo_in = lax.ppermute(halo, ("x", "c", "z"), [(i, i + 1) for i in range(stretches - 1)])
    entry_far = swap_cores(entry_near)
    gathered_far = swap_cores(gathered)
    hloc, acum, ends, total = call(
        gates_kernel,
        idx,
        (xn, halo_in, entry, rows, rw, ew, *entry_near, *entry_far),
        [((4, 256, 128), F32), ((4, 256, 128), F32), ((2, 4, 8, 128), F32), ((2, 4, 4, 128), F32)],
        scratch=[pltpu.VMEM((4, 280, 128), F32)],
    )
    entering = enter(total, flags)
    silu, wo = call(
        prepare_kernel,
        idx,
        (xn, valve, ow, *gathered, *gathered_far),
        [((256, 512), F32), ((512, 2048), BF16)],
        scratch=[pltpu.VMEM((2048, 512), BF16)],
    )
    own, *parts = call(
        output_kernel,
        idx,
        (hloc, acum, ends, entering, silu, wo),
        [((4, 16, 2048), F32)] + [((4, 16, 2048), BF16)] * 3,
        scratch=[pltpu.VMEM((4, 256, 128), F32), pltpu.VMEM((4, 64, 512), BF16)],
    )
    parts = [shift(p, "y", by) for p, by in zip(parts, SHIFTS)]
    (mixed,) = call(mix_kernel, None, (own, *parts), [((4, 16, 2048), BF16)], to_hbm=True)
    return mixed


def solution(mesh):
    finer = Mesh(mesh.devices.reshape(4, 2, 4, 4), SP_TP)
    placed = (
        P(None, SP_TP, None),
        P(),
        P(None, TP),
        P(None, TP),
        P(None, TP),
        P(TP),
        P(TP, None, None),
        P(TP),
        P(TP, None, None),
        P(TP),
        P(TP),
        P(TP, None),
    )

    return jax.shard_map(
        per_device, mesh=finer, in_specs=placed, out_specs=P(None, SP_TP, None), check_vma=False
    )
```
